512 devices in a mesh: grp: 2 (over y), sp: 32 (over z, core), tp: 8 (over x).
Axes of the slice: x: 8, y: 2, z: 16, core: 2. Of those that a mesh axis runs over, the one named last changes fastest.
The devices are a block of a 8x8x16 slice.
Arguments:
- glu_value: bfloat16 [8192, 2048], P(('grp', 'sp'), 'tp'), parts along dimension 0, may hold values from -6 to 6
- glu_gate: bfloat16 [8192, 2048], P(('grp', 'sp'), 'tp'), parts along dimension 0, may hold values from -9 to 9
- segments: int32 [8192], P(('grp', 'sp')), parts along dimension 0, may hold values from 0 to 7, never falling along the last dimension, each value on 1 to 2048 neighbouring positions
- conv_kernel: float32 [31, 2048], P(None, 'tp'), may hold values from -3.5 to 3.5
- norm_gain: float32 [2048], P('tp'), may hold values from 0.1 to 1.9
- norm_bias: float32 [2048], P('tp'), may hold values from -3 to 3
- residual: bfloat16 [8192, 2048], P(('grp', 'sp'), 'tp'), parts along dimension 0, may hold values from -6 to 6
- out_weight: bfloat16 [2048, 2048], P('tp'), may hold values from -0.125 to 0.125
- rms_gain: float32 [2048], replicated, may hold values from 0.1 to 1.9
- experts: int32 [8192, 4], P(('grp', 'sp')), parts along dimension 0, may hold values from 0 to 31, all different within a row; in each aligned block of 128 rows (0 to 127, 128 to 255, ...) at most 32 rows name the same one
- route_weights: float32 [8192, 4], P(('grp', 'sp')), parts along dimension 0, may hold values from 0.1 to 1
- glu_weight: bfloat16 [32, 2048, 2048], P('sp', None, 'tp'), may hold values from -0.5 to 0.5
- lin_weight: bfloat16 [32, 2048, 2048], P('sp', None, 'tp'), may hold values from -0.5 to 0.5
- down_weight: bfloat16 [32, 2048, 2048], P('sp', None, 'tp'), may hold values from -0.015625 to 0.015625
Outputs:
- layer_output: bfloat16 [8192, 2048], P(('grp', 'sp'), 'tp'), parts along dimension 0
The draws below stay inside these ranges and needn't reach their ends.
There are 2 independent parts, one for each index of `grp`. The reference program is written for one: setup_inputs(seed, part) draws one part's arguments, and reference() takes and returns one part's arrays. A program takes and returns all parts, laid end to end along the dimension named above; an argument that names none is the same for every part. Nothing has to cross between parts.
Inputs may be any that keep to these rules, and one draw needn't show every extreme that they name: Each row names 4 different experts. In each aligned block of 128 rows no expert is named by more than 32 rows, and in some block an expert is named by exactly 32 rows. `segments`: never falling along positions; a document holds from 1 up to 2048 positions, and one holds exactly that many.
All inputs are finite; a program needn't handle non-finite values.
Results may differ from the reference program's by a relative error of at most 0.017.
Values may be sent and summed in bfloat16 or wider, within the bound.
No kernel may reach another device: no remote copies, remote signals or barrier semaphores. Data moves between devices by JAX's collectives and lax.ppermute only.
A program may use at most 64 MiB of HBM per device.

```python
import math
import jax
import jax.numpy as jnp
import numpy as np
from jax import lax

D = 2048
FF = 2048
TAPS = 31
TOPK = 4
TOK_DEV = 128
TOKENS = 4096
EXPERTS = 32
CAP = 32
N_SP = 32
N_TP = 8


def draw_conv_kernel(key, part):
    channel = jnp.arange(D, dtype=jnp.float32) / D
    values = jnp.clip(jax.random.normal(key, (TAPS, D), jnp.float32), -4.0, 4.0)
    ramp = 3.0 ** channel
    return values * ramp[None, :] * TAPS ** (-0.5)


def level_of(key, shape, shards, least, largest):
    loudness, own = 1.0, jax.random.fold_in(key, 6)
    for position, shards_of in shards:
        heights = jnp.exp(jax.random.uniform(jax.random.fold_in(own, position), (shards_of,), jnp.float32, least / len(shards), largest / len(shards)))
        loudness = loudness * jnp.repeat(heights, shape[position] // shards_of).reshape([-1 if axis == position else 1 for axis in range(len(shape))])
    return loudness


def split_up(amount, total, most, lean):
    portions = [(1 << 20) // math.isqrt(standing ** lean) + 1 for standing in range(2, amount + 1)]
    surplus, holding = total - most - (amount - 1), [1] * (amount - 1)
    while surplus > 0:
        candidates = [i for i in range(amount - 1) if holding[i] < most]
        mass, budget = sum([portions[i] for i in candidates]), surplus
        for i in candidates:
            extra = min(most - holding[i], max(1, budget * portions[i] // mass), surplus)
            holding[i] = holding[i] + extra
            surplus = surplus - extra
    return np.array([most] + holding)


def uneven(stream_key, number_of, total, limit, skew):
    if number_of == 2:
        one = jax.random.randint(stream_key, (), max(1, total - limit), min(limit, total - 1) + 1)
        return jnp.stack([one, total - one])
    lengths = jnp.asarray(split_up(number_of, total, limit, skew), jnp.int32)
    twos = (number_of - 1) // 2
    source_of, taker = lengths[1:1 + 2 * twos:2], lengths[2:2 + 2 * twos:2]
    margin = jnp.minimum(source_of - 1, limit - taker)
    moved = jax.random.randint(jax.random.fold_in(stream_key, 1), (twos,), 0, 1 << 20) % (margin + 1)
    lengths = lengths.at[1:1 + 2 * twos:2].set(source_of - moved).at[2:2 + 2 * twos:2].set(taker + moved)
    return lengths[jax.random.permutation(jax.random.fold_in(stream_key, 2), number_of)]


def routed_block(key, own, number, rows, count, top, bound, skew):
    order = jax.random.permutation(key, count)
    crowded, ordinary = portions_of(count, rows * top, bound, skew, True), portions_of(count, rows * top, bound, skew, False)
    places = jnp.arange(count)

    def named(lengths, offset_by):
        used = int((lengths > 0).sum())
        fixed = max(1, used // 4)
        moved = fixed + (places - fixed + offset_by * (used - fixed)) % max(1, count - fixed)
        return jnp.zeros((count,), jnp.int32).at[order[jnp.where(places < fixed, places, moved)]].set(jnp.asarray(lengths, jnp.int32))

    lengths = jnp.where(number % 4 == 0, named(crowded, number // 4), named(ordinary, number - number // 4 - 1))
    mixed = jax.random.permutation(jax.random.fold_in(own, 3), count)
    source_of, taker = mixed[0:count // 2 * 2:2], mixed[1:count // 2 * 2:2]
    slack = jnp.minimum(lengths[source_of] - 1, bound - lengths[taker]) // 2
    slack = jnp.where((source_of == order[0]) | (taker == order[0]) | (lengths[taker] == 0), 0, jnp.maximum(slack, 0))
    moved = jax.random.randint(jax.random.fold_in(own, 4), (count // 2,), 0, 1 << 20) % (slack + 1)
    lengths = lengths.at[source_of].add(-moved).at[taker].add(moved)
    members = jnp.searchsorted(jnp.cumsum(lengths), jnp.arange(rows * top), side="right").astype(jnp.int32)
    table = members.reshape(top, rows).T
    table = table[jax.random.permutation(jax.random.fold_in(own, 1), rows)]
    offset_by = jax.random.randint(jax.random.fold_in(own, 2), (rows, 1), 0, top)
    return jnp.take_along_axis(table, (jnp.arange(top)[None, :] + offset_by) % top, axis=1)


def portions_of(number_of, total, bound, slope, full):
    portions = [(1 << 20) // math.isqrt(standing ** slope) + 1 for standing in range(1, number_of + 1)]
    largest = bound if full else min(bound, max(-(-total // number_of), total * portions[0] // sum(portions)))
    least = 1 if total - largest >= number_of - 1 else 0
    holding, surplus = [largest] + [least] * (number_of - 1), total - largest - least * (number_of - 1)
    while surplus > 0:
        candidates = [i for i in range(1, number_of) if holding[i] < largest] or [i for i in range(1, number_of) if holding[i] < bound]
        whole, remaining = sum([portions[i] for i in candidates]), surplus
        for i in candidates:
            more = min(bound - holding[i], max(1, remaining * portions[i] // whole), surplus)
            holding[i] = holding[i] + more
            surplus = surplus - more
    return np.array(holding)


def noise(rng, extent, scale, bound, split=(), held_as=jnp.bfloat16):
    loudness = level_of(rng, extent, split, -0.22, 0.18) if split else 1.0
    values = jax.random.normal(rng, extent, jnp.float32) * scale * loudness
    return jnp.minimum(jnp.maximum(values, -bound), bound).astype(held_as)


def setup_inputs(seed: int = 0, part: int = 0) -> dict:
    seeds = jax.random.split(jax.random.key(seed), 15)
    part_keys = jax.random.split(jax.random.fold_in(seeds[14], part), 15)
    glu_value = noise(part_keys[0], (TOKENS, D), 1.0, 6.0, ((0, 32), (1, 8)))
    glu_gate = noise(part_keys[1], (TOKENS, D), 1.5, 9.0, ((0, 32), (1, 8)))
    segments = jnp.searchsorted(jnp.cumsum(uneven(part_keys[2], max(2, N_SP // 4), TOKENS, TOKENS // 2, 1)), jnp.arange(TOKENS), side="right").astype(jnp.int32)
    conv_kernel = draw_conv_kernel(jax.random.fold_in(seeds[14], 71), part)
    norm_gain = jnp.clip(1.0 + 0.18 * jax.random.normal(seeds[4], (D,), jnp.float32), 0.1, 1.9)
    norm_bias = noise(seeds[5], (D,), 0.5, 3.0, ((0, 8),), jnp.float32)
    residual = noise(part_keys[6], (TOKENS, D), 1.0, 6.0, ((0, 32), (1, 8)))
    out_weight = noise(seeds[7], (D, D), D ** -0.5, 0.125, ((0, 8),))
    rms_gain = jnp.clip(1.0 + 0.18 * jax.random.normal(seeds[8], (D,), jnp.float32), 0.1, 1.9)
    experts_keys = jax.random.split(jax.random.fold_in(part_keys[9], 1), TOKENS // TOK_DEV)
    experts_turns = jax.random.permutation(jax.random.fold_in(part_keys[9], 3), TOKENS // TOK_DEV)
    experts = jax.vmap(lambda own, number: routed_block(jax.random.fold_in(part_keys[9], 2), own, number, TOK_DEV, EXPERTS, TOPK, CAP, 2))(experts_keys, experts_turns).reshape((TOKENS, TOPK))
    route_weights = jnp.clip(jnp.exp(math.log(1.0) - 2.3025851 * jax.random.uniform(part_keys[10], (TOKENS, TOPK), jnp.float32) ** level_of(part_keys[10], (TOKENS, TOPK), ((0, 32),), -0.2, 0.2)), 0.1, 1.0)
    glu_weight = noise(seeds[11], (EXPERTS, D, FF), (D // 16) ** -0.5, 0.5, ((0, 32), (2, 8)))
    lin_weight = noise(seeds[12], (EXPERTS, D, FF), (D // 16) ** -0.5, 0.5, ((0, 32), (2, 8)))
    down_weight = noise(seeds[13], (EXPERTS, FF, D), (FF * 64) ** -0.5, 0.015625, ((0, 32), (2, 8)))
    return dict(glu_value=glu_value, glu_gate=glu_gate, segments=segments, conv_kernel=conv_kernel, norm_gain=norm_gain, norm_bias=norm_bias, residual=residual, out_weight=out_weight, rms_gain=rms_gain, experts=experts, route_weights=route_weights, glu_weight=glu_weight, lin_weight=lin_weight, down_weight=down_weight)


EPSILON = 1e-05
CLAMP_LIMIT = 7.0
SIGMOID_SCALE = 1.702

def clamped_unit(gate_pre, lin_pre):
    gate_clip = jnp.minimum(gate_pre, CLAMP_LIMIT)
    linear = jnp.clip(lin_pre, -CLAMP_LIMIT, CLAMP_LIMIT)
    return gate_clip * jax.nn.sigmoid(SIGMOID_SCALE * gate_clip) * (linear + 1.0)

def reference(glu_value, glu_gate, segments, conv_kernel, norm_gain, norm_bias, residual, out_weight, rms_gain, experts, route_weights, glu_weight, lin_weight, down_weight):
    glu_out = (glu_value.astype(jnp.float32) * jax.nn.sigmoid(glu_gate.astype(jnp.float32))).astype(jnp.bfloat16)
    glu_float = glu_out.astype(jnp.float32)
    conv_sum = jnp.zeros((TOKENS, D), jnp.float32)
    for offset in range(TAPS):
        shifted = jnp.pad(glu_float, ((offset, 0), (0, 0)))[:TOKENS]
        shifted_segments = jnp.pad(segments, (offset, 0), constant_values=-1)[:TOKENS]
        same_document = (shifted_segments == segments).astype(jnp.float32)
        conv_sum = conv_sum + conv_kernel[offset][None, :] * shifted * same_document[:, None]
    row_mean = lax.optimization_barrier(jnp.sum(conv_sum, axis=1, keepdims=True)) / D
    row_var = lax.optimization_barrier(jnp.sum(conv_sum * conv_sum, axis=1, keepdims=True)) / D - row_mean * row_mean
    normed_conv = (conv_sum - row_mean) * lax.rsqrt(row_var + EPSILON) * norm_gain + norm_bias
    swished = jax.nn.silu(normed_conv).astype(jnp.bfloat16)
    local_width = D // N_TP
    conv_out = jnp.zeros((TOKENS, D), jnp.float32)
    for piece_index in range(N_TP):
        lower = piece_index * local_width
        partial_value = jnp.dot(swished[:, lower:lower + local_width], out_weight[lower:lower + local_width], preferred_element_type=jnp.float32)
        conv_out = conv_out + partial_value.astype(jnp.bfloat16).astype(jnp.float32)
    updated = (residual.astype(jnp.float32) + conv_out).astype(jnp.bfloat16)
    updated_float = updated.astype(jnp.float32)
    normed = (updated_float * lax.rsqrt(lax.optimization_barrier(jnp.mean(updated_float * updated_float, axis=1, keepdims=True)) + EPSILON) * rms_gain).astype(jnp.bfloat16)
    normed_pad = jnp.concatenate([normed, jnp.zeros((1, D), jnp.bfloat16)], axis=0)
    flat_experts = experts.reshape(-1)
    flat_weights = jnp.concatenate([route_weights.reshape(-1), jnp.zeros((1,), jnp.float32)])
    slot_rows = N_SP * CAP

    def expert_step(accum_sum, inputs):
        glu_matrix, lin_matrix, down_matrix, expert_id = inputs
        chosen = jnp.nonzero(flat_experts == expert_id, size=slot_rows, fill_value=TOKENS * TOPK)[0].astype(jnp.int32)
        token_ids = (chosen // TOPK).astype(jnp.int32)
        gathered = normed_pad[token_ids]
        gate_pre = jnp.dot(gathered, glu_matrix, preferred_element_type=jnp.float32)
        lin_pre = jnp.dot(gathered, lin_matrix, preferred_element_type=jnp.float32)
        hidden = clamped_unit(gate_pre, lin_pre).astype(jnp.bfloat16)
        result = jnp.dot(hidden, down_matrix, preferred_element_type=jnp.float32).astype(jnp.bfloat16)
        weighted = result.astype(jnp.float32) * flat_weights[chosen][:, None]
        return (accum_sum.at[token_ids].add(weighted), None)
    accum_sum, unused = lax.scan(expert_step, jnp.zeros((TOKENS + 1, D), jnp.float32), (glu_weight, lin_weight, down_weight, jnp.arange(EXPERTS, dtype=jnp.int32)))
    return (updated_float + accum_sum[:TOKENS]).astype(jnp.bfloat16)
```

```python
import functools

import jax
import jax.numpy as jnp
from jax import lax
from jax.experimental import pallas as pl
from jax.experimental.pallas import tpu as pltpu
from jax.sharding import PartitionSpec as P

EPSILON = 1e-05
CLAMP_LIMIT = 7.0
SIGMOID_SCALE = 1.702
PARTS = 2


def shifted(array, axis, by):
    length = lax.axis_size(axis)
    return lax.ppermute(array, axis, [(i, (i + by) % length) for i in range(length)])


def ring_gather(own, axis, flip):
    length = lax.axis_size(axis)
    step = -1 if flip else 1
    blocks, offsets = [own], [0]
    ahead = back = own
    for hop in range(1, length // 2 + 1):
        ahead = shifted(ahead, axis, step)
        blocks.append(ahead)
        offsets.append(-step * hop)
        if hop < length - length // 2:
            back = shifted(back, axis, -step)
            blocks.append(back)
            offsets.append(step * hop)
    return blocks, tuple(offsets)


def in_blocks(array, dim, length):
    lengths = array.shape
    blocks = array.reshape(*lengths[:dim], length, lengths[dim] // length, *lengths[dim + 1 :])
    return jnp.moveaxis(blocks, dim, 0)


def everyones_sum(array, axis):
    copies = jnp.broadcast_to(array, (lax.axis_size(axis), *array.shape))
    return lax.all_to_all(copies, axis, split_axis=0, concat_axis=0, tiled=True).sum(axis=0)


def clamped_unit(gate_pre, lin_pre):
    gate_clip = jnp.minimum(gate_pre, CLAMP_LIMIT)
    linear = jnp.clip(lin_pre, -CLAMP_LIMIT, CLAMP_LIMIT)
    return gate_clip * jax.nn.sigmoid(SIGMOID_SCALE * gate_clip) * (linear + 1.0)


def hidden_kernel(offsets, tile, me_ref, gain_ref, gate_ref, lin_ref, *refs):
    blocks, out_ref = refs[:-1], refs[-1]
    count = len(blocks)
    rows, width = blocks[0].shape
    owners = [lax.rem(me_ref[0] + offset + count, count) for offset in offsets]

    @pl.loop(0, rows // tile)
    def _(i):
        here = pl.ds(pl.multiple_of(i * tile, tile), tile)
        gate_pre = lin_pre = squares = None
        for block, owner in zip(blocks, owners):
            piece = pl.ds(pl.multiple_of(owner * width, width), width)
            values = block[here, :].astype(jnp.float32)
            square = values * values
            scaled = (values * gain_ref[owner]).astype(jnp.bfloat16)
            gate = jnp.dot(scaled, gate_ref[piece, :], preferred_element_type=jnp.float32)
            lin = jnp.dot(scaled, lin_ref[piece, :], preferred_element_type=jnp.float32)
            squares = square if squares is None else squares + square
            gate_pre = gate if gate_pre is None else gate_pre + gate
            lin_pre = lin if lin_pre is None else lin_pre + lin
        mean = jnp.sum(squares, axis=1, keepdims=True) / (count * width)
        factor = lax.rsqrt(mean + EPSILON)
        out_ref[here, :] = clamped_unit(gate_pre * factor, lin_pre * factor).astype(jnp.bfloat16)


def down_kernel(offsets, tile, me_ref, down_ref, *refs):
    blocks, out_ref = refs[:-1], refs[-1]
    count = len(blocks)
    rows, width = blocks[0].shape
    owners = [lax.rem(me_ref[0] + offset + count, count) for offset in offsets]

    @pl.loop(0, rows // tile)
    def _(i):
        here = pl.ds(pl.multiple_of(i * tile, tile), tile)
        total = None
        for block, owner in zip(blocks, owners):
            piece = pl.ds(pl.multiple_of(owner * width, width), width)
            term = jnp.dot(block[here, :], down_ref[piece, :], preferred_element_type=jnp.float32)
            total = term if total is None else total + term
        out_ref[here, :] = total.astype(jnp.bfloat16)


def local_call(kernel, out_shape, operands, flops):
    smem, vmem = pl.BlockSpec(memory_space=pltpu.SMEM), pl.BlockSpec(memory_space=pltpu.VMEM)
    return pl.pallas_call(
        kernel,
        out_shape=out_shape,
        in_specs=[smem] + [vmem] * (len(operands) - 1),
        out_specs=vmem,
        compiler_params=pltpu.CompilerParams(vmem_limit_bytes=24 * 2**20),
        cost_estimate=pl.CostEstimate(flops=flops, bytes_accessed=2**22, transcendentals=0),
    )(*operands)


def shards(
    glu_value,
    glu_gate,
    segments,
    conv_kernel,
    norm_gain,
    norm_bias,
    residual,
    out_weight,
    rms_gain,
    experts,
    route_weights,
    glu_weight,
    lin_weight,
    down_weight,
):
    bf16, f32 = jnp.bfloat16, jnp.float32
    tok_count, local_width = glu_value.shape
    model_width = out_weight.shape[1]
    reach = conv_kernel.shape[0] - 1
    top_count = experts.shape[1]
    sp_count, tp_count = lax.axis_size("sp"), lax.axis_size("tp")
    expert_total = glu_weight.shape[0] * sp_count
    capacity = min(tok_count, 2 * tok_count * top_count // expert_total)
    me = lax.axis_index("tp").astype(jnp.int32).reshape(1)

    glu_out = (glu_value.astype(f32) * jax.nn.sigmoid(glu_gate.astype(f32))).astype(bf16)
    last_docs = jnp.pad(segments[tok_count - reach :].astype(bf16), (0, local_width - reach))
    tail = jnp.concatenate([glu_out[tok_count - reach :], last_docs[None, :]], axis=0)
    before = lax.ppermute(tail, "sp", [(i, i + 1) for i in range(sp_count - 1)])
    prev_rows, prev_segments = before[:reach], before[reach, :reach].astype(jnp.int32)

    each = jnp.arange(expert_total, dtype=jnp.int32)
    named = experts[:, :, None] == each
    one_hot = jnp.any(named, axis=1)
    weight_of = jnp.sum(jnp.where(named, route_weights[:, :, None], 0.0), axis=1)
    position = jnp.arange(tok_count, dtype=jnp.int32)
    earlier = (position[:, None] > position[None, :]).astype(bf16)
    rank = jnp.dot(earlier, one_hot.astype(bf16), preferred_element_type=f32)
    rank = jnp.where(one_hot, rank, -1.0).astype(bf16)
    slots = capacity // PARTS
    column = jnp.arange(expert_total * slots, dtype=jnp.int32)
    spread = (each[:, None] == column[None, :] // slots).astype(bf16)
    rank_of = jnp.dot(rank, spread, preferred_element_type=f32)
    weight_at = jnp.dot(weight_of, spread.astype(f32), precision=lax.Precision.HIGHEST)
    picks, weights = [], []
    for part in range(PARTS):
        pick = rank_of == (column % slots + part * slots).astype(f32)
        picks.append(pick.astype(bf16))
        weight = jnp.where(pick, weight_at, 0.0)
        upper = lax.reduce_precision(weight, 8, 7)
        weights.append((upper.astype(bf16), (weight - upper).astype(bf16)))

    padded = jnp.concatenate([prev_rows, glu_out], axis=0).astype(f32)
    padded_segments = jnp.concatenate([prev_segments, segments], axis=0)
    conv_sum = jnp.zeros((tok_count, local_width), f32)
    for offset in range(reach + 1):
        lower = reach - offset
        window_rows = padded[lower : lower + tok_count]
        same_document = (padded_segments[lower : lower + tok_count] == segments).astype(f32)
        conv_sum = conv_sum + conv_kernel[offset][None, :] * window_rows * same_document[:, None]
    sums = jnp.concatenate([jnp.sum(conv_sum, axis=1), jnp.sum(conv_sum * conv_sum, axis=1)])
    totals = everyones_sum(sums, "tp")
    row_mean = totals[:tok_count] / model_width
    row_var = totals[tok_count:] / model_width - row_mean * row_mean
    normed_conv = (conv_sum - row_mean[:, None]) * lax.rsqrt(row_var + EPSILON)[
        :, None
    ] * norm_gain + norm_bias
    swished = jax.nn.silu(normed_conv).astype(bf16)
    projected = jnp.dot(swished, out_weight, preferred_element_type=f32).astype(bf16)
    pieces = lax.all_to_all(in_blocks(projected, 1, tp_count), "tp", 0, 0, tiled=True)
    conv_out = jnp.sum(pieces.astype(f32), axis=0)
    updated = (residual.astype(f32) + conv_out).astype(bf16)

    gain = rms_gain.reshape(tp_count, 1, local_width)
    rows = sp_count * slots
    sent = []
    for part in range(PARTS):
        packed = lax.dot_general(
            picks[part], updated, (((0,), (0,)), ((), ())), preferred_element_type=f32
        ).astype(bf16)
        packed = packed.reshape(sp_count, slots, local_width)
        sent.append(lax.all_to_all(packed, "sp", 0, 0, tiled=True).reshape(rows, local_width))
    out_block = jax.ShapeDtypeStruct((rows, local_width), bf16)
    flops = 2 * rows * model_width * local_width
    hidden = []
    for part in range(PARTS):
        blocks, offsets = ring_gather(sent[part], "tp", part % 2)
        hidden.append(
            local_call(
                functools.partial(hidden_kernel, offsets, 128),
                out_block,
                (me, gain, glu_weight[0], lin_weight[0], *blocks),
                2 * flops,
            )
        )
    routed = updated.astype(f32)
    for part in range(PARTS):
        blocks, offsets = ring_gather(hidden[part], "tp", part % 2)
        result = local_call(
            functools.partial(down_kernel, offsets, 128),
            out_block,
            (me, down_weight[0], *blocks),
            flops,
        )
        returned = lax.all_to_all(
            result.reshape(sp_count, slots, local_width), "sp", 0, 0, tiled=True
        ).reshape(rows, local_width)
        for weight in weights[part]:
            routed = routed + jnp.dot(weight, returned, preferred_element_type=f32)
    return routed.astype(bf16)


def solution(mesh):
    in_specs = (
        P(("grp", "sp"), "tp"),
        P(("grp", "sp"), "tp"),
        P(("grp", "sp")),
        P(None, "tp"),
        P("tp"),
        P("tp"),
        P(("grp", "sp"), "tp"),
        P("tp", None),
        P(),
        P(("grp", "sp"), None),
        P(("grp", "sp"), None),
        P("sp", None, "tp"),
        P("sp", None, "tp"),
        P("sp", None, "tp"),
    )
    out_specs = P(("grp", "sp"), "tp")
    return jax.shard_map(shards, mesh=mesh, in_specs=in_specs, out_specs=out_specs, check_vma=False)
```

```python
import functools

import jax
import jax.numpy as jnp
from jax import lax
from jax.experimental import pallas as pl
from jax.experimental.pallas import tpu as pltpu
from jax.sharding import PartitionSpec as P

EPSILON = 1e-05
CLAMP_LIMIT = 7.0
SIGMOID_SCALE = 1.702
PARTS = 2


def shifted(array, axis, by):
    length = lax.axis_size(axis)
    return lax.ppermute(array, axis, [(i, (i + by) % length) for i in range(length)])


def ring_gather(own, axis, flip):
    length = lax.axis_size(axis)
    step = -1 if flip else 1
    blocks, offsets = [own], [0]
    ahead = back = own
    for hop in range(1, length // 2 + 1):
        ahead = shifted(ahead, axis, step)
        blocks.append(ahead)
        offsets.append(-step * hop)
        if hop < length - length // 2:
            back = shifted(back, axis, -step)
            blocks.append(back)
            offsets.append(step * hop)
    return blocks, tuple(offsets)


def in_blocks(array, dim, length):
    lengths = array.shape
    blocks = array.reshape(*lengths[:dim], length, lengths[dim] // length, *lengths[dim + 1 :])
    return jnp.moveaxis(blocks, dim, 0)


def everyones_sum(array, axis):
    copies = jnp.broadcast_to(array, (lax.axis_size(axis), *array.shape))
    return lax.all_to_all(copies, axis, split_axis=0, concat_axis=0, tiled=True).sum(axis=0)


def clamped_unit(gate_pre, lin_pre):
    gate_clip = jnp.minimum(gate_pre, CLAMP_LIMIT)
    linear = jnp.clip(lin_pre, -CLAMP_LIMIT, CLAMP_LIMIT)
    return gate_clip * jax.nn.sigmoid(SIGMOID_SCALE * gate_clip) * (linear + 1.0)


def hidden_kernel(offsets, tile, me_ref, gain_ref, gate_ref, lin_ref, *refs):
    blocks, out_ref = refs[:-1], refs[-1]
    count = len(blocks)
    rows, width = blocks[0].shape
    owners = [lax.rem(me_ref[0] + offset + count, count) for offset in offsets]

    @pl.loop(0, rows // tile)
    def _(i):
        here = pl.ds(pl.multiple_of(i * tile, tile), tile)
        gate_pre = lin_pre = squares = None
        for block, owner in zip(blocks, owners):
            piece = pl.ds(pl.multiple_of(owner * width, width), width)
            values = block[here, :].astype(jnp.float32)
            square = values * values
            scaled = (values * gain_ref[owner]).astype(jnp.bfloat16)
            gate = jnp.dot(scaled, gate_ref[piece, :], preferred_element_type=jnp.float32)
            lin = jnp.dot(scaled, lin_ref[piece, :], preferred_element_type=jnp.float32)
            squares = square if squares is None else squares + square
            gate_pre = gate if gate_pre is None else gate_pre + gate
            lin_pre = lin if lin_pre is None else lin_pre + lin
        mean = jnp.sum(squares, axis=1, keepdims=True) / (count * width)
        factor = lax.rsqrt(mean + EPSILON)
        out_ref[here, :] = clamped_unit(gate_pre * factor, lin_pre * factor).astype(jnp.bfloat16)


def down_kernel(offsets, tile, me_ref, down_ref, *refs):
    blocks, out_ref = refs[:-1], refs[-1]
    count = len(blocks)
    rows, width = blocks[0].shape
    owners = [lax.rem(me_ref[0] + offset + count, count) for offset in offsets]

    @pl.loop(0, rows // tile)
    def _(i):
        here = pl.ds(pl.multiple_of(i * tile, tile), tile)
        total = None
        for block, owner in zip(blocks, owners):
            piece = pl.ds(pl.multiple_of(owner * width, width), width)
            term = jnp.dot(block[here, :], down_ref[piece, :], preferred_element_type=jnp.float32)
            total = term if total is None else total + term
        out_ref[here, :] = total.astype(jnp.bfloat16)


def local_call(kernel, out_shape, operands, flops):
    smem, vmem = pl.BlockSpec(memory_space=pltpu.SMEM), pl.BlockSpec(memory_space=pltpu.VMEM)
    return pl.pallas_call(
        kernel,
        out_shape=out_shape,
        in_specs=[smem] + [vmem] * (len(operands) - 1),
        out_specs=vmem,
        compiler_params=pltpu.CompilerParams(vmem_limit_bytes=24 * 2**20),
        cost_estimate=pl.CostEstimate(flops=flops, bytes_accessed=2**22, transcendentals=0),
    )(*operands)


def shards(
    glu_value,
    glu_gate,
    segments,
    conv_kernel,
    norm_gain,
    norm_bias,
    residual,
    out_weight,
    rms_gain,
    experts,
    route_weights,
    glu_weight,
    lin_weight,
    down_weight,
):
    bf16, f32 = jnp.bfloat16, jnp.float32
    tok_count, local_width = glu_value.shape
    model_width = out_weight.shape[1]
    reach = conv_kernel.shape[0] - 1
    top_count = experts.shape[1]
    sp_count, tp_count = lax.axis_size("sp"), lax.axis_size("tp")
    expert_total = glu_weight.shape[0] * sp_count
    capacity = min(tok_count, 2 * tok_count * top_count // expert_total)
    me = lax.axis_index("tp").astype(jnp.int32).reshape(1)

    glu_out = (glu_value.astype(f32) * jax.nn.sigmoid(glu_gate.astype(f32))).astype(bf16)
    last_docs = jnp.pad(segments[tok_count - reach :].astype(bf16), (0, local_width - reach))
    tail = jnp.concatenate([glu_out[tok_count - reach :], last_docs[None, :]], axis=0)
    before = lax.ppermute(tail, "sp", [(i, i + 1) for i in range(sp_count - 1)])
    prev_rows, prev_segments = before[:reach], before[reach, :reach].astype(jnp.int32)

    each = jnp.arange(expert_total, dtype=jnp.int32)
    named = experts[:, :, None] == each
    one_hot = jnp.any(named, axis=1)
    weight_of = jnp.sum(jnp.where(named, route_weights[:, :, None], 0.0), axis=1)
    position = jnp.arange(tok_count, dtype=jnp.int32)
    earlier = (position[:, None] > position[None, :]).astype(bf16)
    rank = jnp.dot(earlier, one_hot.astype(bf16), preferred_element_type=f32)
    rank = jnp.where(one_hot, rank, -1.0).astype(bf16)
    column = jnp.arange(expert_total * capacity, dtype=jnp.int32)
    spread = (each[:, None] == column[None, :] // capacity).astype(bf16)
    rank_of = jnp.dot(rank, spread, preferred_element_type=f32)
    weight_at = jnp.dot(weight_of, spread.astype(f32), precision=lax.Precision.HIGHEST)
    pick = rank_of == (column % capacity).astype(f32)
    weight = jnp.where(pick, weight_at, 0.0)
    upper = lax.reduce_precision(weight, 8, 7)
    weights = (upper.astype(bf16), (weight - upper).astype(bf16))

    padded = jnp.concatenate([prev_rows, glu_out], axis=0).astype(f32)
    padded_segments = jnp.concatenate([prev_segments, segments], axis=0)
    conv_sum = jnp.zeros((tok_count, local_width), f32)
    for offset in range(reach + 1):
        lower = reach - offset
        window_rows = padded[lower : lower + tok_count]
        same_document = (padded_segments[lower : lower + tok_count] == segments).astype(f32)
        conv_sum = conv_sum + conv_kernel[offset][None, :] * window_rows * same_document[:, None]
    sums = jnp.concatenate([jnp.sum(conv_sum, axis=1), jnp.sum(conv_sum * conv_sum, axis=1)])
    totals = everyones_sum(sums, "tp")
    row_mean = totals[:tok_count] / model_width
    row_var = totals[tok_count:] / model_width - row_mean * row_mean
    normed_conv = (conv_sum - row_mean[:, None]) * lax.rsqrt(row_var + EPSILON)[
        :, None
    ] * norm_gain + norm_bias
    swished = jax.nn.silu(normed_conv).astype(bf16)
    projected = jnp.dot(swished, out_weight, preferred_element_type=f32).astype(bf16)
    pieces = lax.all_to_all(in_blocks(projected, 1, tp_count), "tp", 0, 0, tiled=True)
    conv_out = jnp.sum(pieces.astype(f32), axis=0)
    updated = (residual.astype(f32) + conv_out).astype(bf16)

    gain = rms_gain.reshape(tp_count, 1, local_width)
    rows = sp_count * capacity
    packed = lax.dot_general(
        pick.astype(bf16), updated, (((0,), (0,)), ((), ())), preferred_element_type=f32
    ).astype(bf16)
    packed = packed.reshape(sp_count, capacity, local_width)
    arrived = lax.all_to_all(packed, "sp", 0, 0, tiled=True).reshape(rows, local_width)
    part_rows = rows // PARTS
    out_block = jax.ShapeDtypeStruct((part_rows, local_width), bf16)
    flops = 2 * part_rows * model_width * local_width
    hidden, results = [], []
    for part in range(PARTS):
        own = arrived[part * part_rows : (part + 1) * part_rows]
        blocks, offsets = ring_gather(own, "tp", part % 2)
        hidden.append(
            local_call(
                functools.partial(hidden_kernel, offsets, 128),
                out_block,
                (me, gain, glu_weight[0], lin_weight[0], *blocks),
                2 * flops,
            )
        )
    for part in range(PARTS):
        blocks, offsets = ring_gather(hidden[part], "tp", part % 2)
        results.append(
            local_call(
                functools.partial(down_kernel, offsets, 128),
                out_block,
                (me, down_weight[0], *blocks),
                flops,
            )
        )
    result = jnp.concatenate(results, axis=0).reshape(sp_count, capacity, local_width)
    returned = lax.all_to_all(result, "sp", 0, 0, tiled=True).reshape(rows, local_width)
    routed = updated.astype(f32)
    for weight in weights:
        routed = routed + jnp.dot(weight, returned, preferred_element_type=f32)
    return routed.astype(bf16)


def solution(mesh):
    in_specs = (
        P(("grp", "sp"), "tp"),
        P(("grp", "sp"), "tp"),
        P(("grp", "sp")),
        P(None, "tp"),
        P("tp"),
        P("tp"),
        P(("grp", "sp"), "tp"),
        P("tp", None),
        P(),
        P(("grp", "sp"), None),
        P(("grp", "sp"), None),
        P("sp", None, "tp"),
        P("sp", None, "tp"),
        P("sp", None, "tp"),
    )
    out_specs = P(("grp", "sp"), "tp")
    return jax.shard_map(shards, mesh=mesh, in_specs=in_specs, out_specs=out_specs, check_vma=False)
```

```python
import functools

import jax
import jax.numpy as jnp
from jax import lax
from jax.experimental import pallas as pl
from jax.experimental.pallas import tpu as pltpu
from jax.sharding import PartitionSpec as P

EPSILON = 1e-05
CLAMP_LIMIT = 7.0
SIGMOID_SCALE = 1.702


def shifted(array, axis, by):
    length = lax.axis_size(axis)
    return lax.ppermute(array, axis, [(i, (i + by) % length) for i in range(length)])


def ring_gather(own, axis):
    half = lax.axis_size(axis) // 2
    blocks, offsets = [own], [0]
    ahead = back = own
    for hop in range(1, half):
        ahead, back = shifted(ahead, axis, 1), shifted(back, axis, -1)
        blocks += [ahead, back]
        offsets += [-hop, hop]
    middle = own.shape[0] // 2
    last = (shifted(ahead[:middle], axis, 1), shifted(back[middle:], axis, -1))
    return blocks, tuple(offsets), last


def in_blocks(array, dim, length):
    lengths = array.shape
    blocks = array.reshape(*lengths[:dim], length, lengths[dim] // length, *lengths[dim + 1 :])
    return jnp.moveaxis(blocks, dim, 0)


def everyones_sum(array, axis):
    copies = jnp.broadcast_to(array, (lax.axis_size(axis), *array.shape))
    return lax.all_to_all(copies, axis, split_axis=0, concat_axis=0, tiled=True).sum(axis=0)


def clamped_unit(gate_pre, lin_pre):
    gate_clip = jnp.minimum(gate_pre, CLAMP_LIMIT)
    linear = jnp.clip(lin_pre, -CLAMP_LIMIT, CLAMP_LIMIT)
    return gate_clip * jax.nn.sigmoid(SIGMOID_SCALE * gate_clip) * (linear + 1.0)


def whole_rows(halves, here):
    rows = halves[0].shape[0]
    at = here.start % rows
    return halves[here.start // rows][at : at + here.size, :]


def owner_of(me_ref, offset, count):
    return lax.rem(me_ref[0] + offset + count, count)


def expand_terms(values, owner, gain_ref, gate_ref, lin_ref):
    width = values.shape[1]
    piece = pl.ds(pl.multiple_of(owner * width, width), width)
    values = values.astype(jnp.float32)
    scaled = (values * gain_ref[owner]).astype(jnp.bfloat16)
    gate = jnp.dot(scaled, gate_ref[piece, :], preferred_element_type=jnp.float32)
    lin = jnp.dot(scaled, lin_ref[piece, :], preferred_element_type=jnp.float32)
    lanes = gate_ref.shape[1] // 2
    squares = values * values
    return gate, lin, squares[:, :lanes] + squares[:, lanes:]


def added(totals, terms):
    return terms if totals is None else tuple(a + b for a, b in zip(totals, terms))


def expand_kernel(count, offsets, tile, me_ref, gain_ref, gate_ref, lin_ref, *refs):
    blocks, outs = refs[: len(offsets)], refs[len(offsets) :]
    owners = [owner_of(me_ref, offset, count) for offset in offsets]
    for start in range(0, blocks[0].shape[0], tile):
        here, totals = pl.ds(start, tile), None
        for block, owner in zip(blocks, owners):
            terms = expand_terms(block[here, :], owner, gain_ref, gate_ref, lin_ref)
            totals = added(totals, terms)
        for out, total in zip(outs, totals):
            out[here, :] = total


def hidden_kernel(count, tile, me_ref, gain_ref, gate_ref, lin_ref, *refs):
    halves, sums, out_ref = refs[:2], refs[2:5], refs[5]
    owner = owner_of(me_ref, count // 2, count)
    for start in range(0, out_ref.shape[0], tile):
        here = pl.ds(start, tile)
        terms = expand_terms(whole_rows(halves, here), owner, gain_ref, gate_ref, lin_ref)
        gate, lin, squares = added(tuple(ref[here, :] for ref in sums), terms)
        mean = jnp.sum(squares, axis=1, keepdims=True) / (count * out_ref.shape[1])
        factor = lax.rsqrt(mean + EPSILON)
        out_ref[here, :] = clamped_unit(gate * factor, lin * factor).astype(jnp.bfloat16)


def down_term(values, owner, down_ref):
    width = values.shape[1]
    piece = pl.ds(pl.multiple_of(owner * width, width), width)
    return jnp.dot(values, down_ref[piece, :], preferred_element_type=jnp.float32)


def down_kernel(count, offsets, tile, me_ref, down_ref, *refs):
    blocks, out_ref = refs[:-1], refs[-1]
    owners = [owner_of(me_ref, offset, count) for offset in offsets]
    for start in range(0, out_ref.shape[0], tile):
        here, total = pl.ds(start, tile), None
        for block, owner in zip(blocks, owners):
            term = down_term(block[here, :], owner, down_ref)
            total = term if total is None else total + term
        out_ref[here, :] = total


def result_kernel(count, tile, me_ref, down_ref, top_ref, low_ref, sum_ref, out_ref):
    owner = owner_of(me_ref, count // 2, count)
    for start in range(0, out_ref.shape[0], tile):
        here = pl.ds(start, tile)
        term = down_term(whole_rows((top_ref, low_ref), here), owner, down_ref)
        out_ref[here, :] = (sum_ref[here, :] + term).astype(jnp.bfloat16)


def local_call(kernel, out_shape, operands, flops):
    smem, vmem = pl.BlockSpec(memory_space=pltpu.SMEM), pl.BlockSpec(memory_space=pltpu.VMEM)
    return pl.pallas_call(
        kernel,
        out_shape=out_shape,
        in_specs=[smem] + [vmem] * (len(operands) - 1),
        out_specs=[vmem] * len(out_shape) if isinstance(out_shape, list) else vmem,
        compiler_params=pltpu.CompilerParams(vmem_limit_bytes=24 * 2**20),
        cost_estimate=pl.CostEstimate(flops=flops, bytes_accessed=2**22, transcendentals=0),
    )(*operands)


def shards(
    glu_value,
    glu_gate,
    segments,
    conv_kernel,
    norm_gain,
    norm_bias,
    residual,
    out_weight,
    rms_gain,
    experts,
    route_weights,
    glu_weight,
    lin_weight,
    down_weight,
):
    bf16, f32 = jnp.bfloat16, jnp.float32
    tok_count, local_width = glu_value.shape
    model_width = out_weight.shape[1]
    reach = conv_kernel.shape[0] - 1
    top_count = experts.shape[1]
    sp_count, tp_count = lax.axis_size("sp"), lax.axis_size("tp")
    expert_total = glu_weight.shape[0] * sp_count
    capacity = min(tok_count, 2 * tok_count * top_count // expert_total)
    me = lax.axis_index("tp").astype(jnp.int32).reshape(1)
    me, glu_value = lax.optimization_barrier((me, glu_value))

    glu_out = (glu_value.astype(f32) * jax.nn.sigmoid(glu_gate.astype(f32))).astype(bf16)
    last_docs = jnp.pad(segments[tok_count - reach :].astype(bf16), (0, local_width - reach))
    tail = jnp.concatenate([glu_out[tok_count - reach :], last_docs[None, :]], axis=0)
    before = lax.ppermute(tail, "sp", [(i, i + 1) for i in range(sp_count - 1)])
    prev_rows, prev_segments = before[:reach], before[reach, :reach].astype(jnp.int32)

    each = jnp.arange(expert_total, dtype=jnp.int32)
    named = experts[:, :, None] == each
    one_hot = jnp.any(named, axis=1)
    weight_of = jnp.sum(jnp.where(named, route_weights[:, :, None], 0.0), axis=1)
    position = jnp.arange(tok_count, dtype=jnp.int32)
    earlier = (position[:, None] > position[None, :]).astype(bf16)
    rank = jnp.dot(earlier, one_hot.astype(bf16), preferred_element_type=f32)
    rank = jnp.where(one_hot, rank, -1.0).astype(bf16)
    column = jnp.arange(expert_total * capacity, dtype=jnp.int32)
    spread = (each[:, None] == column[None, :] // capacity).astype(bf16)
    rank_of = jnp.dot(rank, spread, preferred_element_type=f32)
    weight_at = jnp.dot(weight_of, spread.astype(f32), precision=lax.Precision.HIGHEST)
    pick = rank_of == (column % capacity).astype(f32)
    weight = jnp.where(pick, weight_at, 0.0)
    upper = lax.reduce_precision(weight, 8, 7)
    weights = (upper.astype(bf16), (weight - upper).astype(bf16))

    padded = jnp.concatenate([prev_rows, glu_out], axis=0).astype(f32)
    padded_segments = jnp.concatenate([prev_segments, segments], axis=0)
    conv_sum = jnp.zeros((tok_count, local_width), f32)
    for offset in range(reach + 1):
        lower = reach - offset
        window_rows = padded[lower : lower + tok_count]
        same_document = (padded_segments[lower : lower + tok_count] == segments).astype(f32)
        conv_sum = conv_sum + conv_kernel[offset][None, :] * window_rows * same_document[:, None]
    sums = jnp.concatenate([jnp.sum(conv_sum, axis=1), jnp.sum(conv_sum * conv_sum, axis=1)])
    totals = everyones_sum(sums, "tp")
    row_mean = totals[:tok_count] / model_width
    row_var = totals[tok_count:] / model_width - row_mean * row_mean
    normed_conv = (conv_sum - row_mean[:, None]) * lax.rsqrt(row_var + EPSILON)[
        :, None
    ] * norm_gain + norm_bias
    swished = jax.nn.silu(normed_conv).astype(bf16)
    projected = jnp.dot(swished, out_weight, preferred_element_type=f32).astype(bf16)
    pieces = lax.all_to_all(in_blocks(projected, 1, tp_count), "tp", 0, 0, tiled=True)
    conv_out = jnp.sum(pieces.astype(f32), axis=0)
    updated = (residual.astype(f32) + conv_out).astype(bf16)

    gain = rms_gain.reshape(tp_count, 1, local_width)
    rows = sp_count * capacity
    packed = lax.dot_general(
        pick.astype(bf16), updated, (((0,), (0,)), ((), ())), preferred_element_type=f32
    ).astype(bf16)
    packed = packed.reshape(sp_count, capacity, local_width)
    arrived = lax.all_to_all(packed, "sp", 0, 0, tiled=True).reshape(rows, local_width)
    tile = min(rows // 2, 256)
    flops = 2 * rows * model_width * local_width
    sums = jax.ShapeDtypeStruct((rows, local_width), f32)
    squares = jax.ShapeDtypeStruct((rows, local_width // 2), f32)
    out = jax.ShapeDtypeStruct((rows, local_width), bf16)
    weights_in = (me, gain, glu_weight[0], lin_weight[0])
    blocks, offsets, last = ring_gather(arrived, "tp")
    expand = functools.partial(expand_kernel, tp_count, offsets, tile)
    partial = local_call(expand, [sums, sums, squares], (*weights_in, *blocks), 2 * flops)
    finish = functools.partial(hidden_kernel, tp_count, tile)
    hidden = local_call(finish, out, (*weights_in, *last, *partial), flops // tp_count)
    blocks, offsets, last = ring_gather(hidden, "tp")
    down = functools.partial(down_kernel, tp_count, offsets, tile)
    partial = local_call(down, sums, (me, down_weight[0], *blocks), flops)
    finish = functools.partial(result_kernel, tp_count, tile)
    result = local_call(finish, out, (me, down_weight[0], *last, partial), flops // tp_count)
    result = result.reshape(sp_count, capacity, local_width)
    returned = lax.all_to_all(result, "sp", 0, 0, tiled=True).reshape(rows, local_width)
    routed = updated.astype(f32)
    for weight in weights:
        routed = routed + jnp.dot(weight, returned, preferred_element_type=f32)
    return routed.astype(bf16)


def solution(mesh):
    in_specs = (
        P(("grp", "sp"), "tp"),
        P(("grp", "sp"), "tp"),
        P(("grp", "sp")),
        P(None, "tp"),
        P("tp"),
        P("tp"),
        P(("grp", "sp"), "tp"),
        P("tp", None),
        P(),
        P(("grp", "sp"), None),
        P(("grp", "sp"), None),
        P("sp", None, "tp"),
        P("sp", None, "tp"),
        P("sp", None, "tp"),
    )
    out_specs = P(("grp", "sp"), "tp")
    return jax.shard_map(shards, mesh=mesh, in_specs=in_specs, out_specs=out_specs, check_vma=False)
```

```python
import functools

import jax
import jax.numpy as jnp
from jax import lax
from jax.experimental import pallas as pl
from jax.experimental.pallas import tpu as pltpu
from jax.sharding import PartitionSpec as P

EPSILON = 1e-05
CLAMP_LIMIT = 7.0
SIGMOID_SCALE = 1.702


def shifted(array, axes, by):
    lines, length = (lax.axis_size(axis) for axis in axes)
    pairs = [
        (line * length + i, line * length + (i + (-by if line % 2 else by)) % length)
        for line in range(lines)
        for i in range(length)
    ]
    return lax.ppermute(array, axes, pairs)


def ring_gather(own, axes):
    half = lax.axis_size(axes[-1]) // 2
    blocks, offsets = [own], [0]
    ahead = back = own
    for hop in range(1, half):
        ahead, back = shifted(ahead, axes, 1), shifted(back, axes, -1)
        blocks += [ahead, back]
        offsets += [-hop, hop]
    middle = own.shape[0] // 2
    last = (shifted(ahead[:middle], axes, 1), shifted(back[middle:], axes, -1))
    return blocks, tuple(offsets), last


def in_blocks(array, dim, length):
    lengths = array.shape
    blocks = array.reshape(*lengths[:dim], length, lengths[dim] // length, *lengths[dim + 1 :])
    return jnp.moveaxis(blocks, dim, 0)


def everyones_sum(array, axis):
    copies = jnp.broadcast_to(array, (lax.axis_size(axis), *array.shape))
    return lax.all_to_all(copies, axis, split_axis=0, concat_axis=0, tiled=True).sum(axis=0)


def clamped_unit(gate_pre, lin_pre):
    gate_clip = jnp.minimum(gate_pre, CLAMP_LIMIT)
    linear = jnp.clip(lin_pre, -CLAMP_LIMIT, CLAMP_LIMIT)
    return gate_clip * jax.nn.sigmoid(SIGMOID_SCALE * gate_clip) * (linear + 1.0)


def whole_rows(halves, here):
    rows = halves[0].shape[0]
    at = here.start % rows
    return halves[here.start // rows][at : at + here.size, :]


def owner_of(me_ref, offset, count):
    return lax.rem(me_ref[0] + offset * me_ref[1] + count, count)


def expand_terms(values, owner, gain_ref, gate_ref, lin_ref):
    width = values.shape[1]
    piece = pl.ds(pl.multiple_of(owner * width, width), width)
    values = values.astype(jnp.float32)
    scaled = (values * gain_ref[owner]).astype(jnp.bfloat16)
    gate = jnp.dot(scaled, gate_ref[piece, :], preferred_element_type=jnp.float32)
    lin = jnp.dot(scaled, lin_ref[piece, :], preferred_element_type=jnp.float32)
    lanes = gate_ref.shape[1] // 2
    squares = values * values
    return gate, lin, squares[:, :lanes] + squares[:, lanes:]


def added(totals, terms):
    return terms if totals is None else tuple(a + b for a, b in zip(totals, terms))


def expand_kernel(count, offsets, tile, me_ref, gain_ref, gate_ref, lin_ref, *refs):
    blocks, outs = refs[: len(offsets)], refs[len(offsets) :]
    owners = [owner_of(me_ref, offset, count) for offset in offsets]
    for start in range(0, blocks[0].shape[0], tile):
        here, totals = pl.ds(start, tile), None
        for block, owner in zip(blocks, owners):
            terms = expand_terms(block[here, :], owner, gain_ref, gate_ref, lin_ref)
            totals = added(totals, terms)
        for out, total in zip(outs, totals):
            out[here, :] = total


def hidden_kernel(count, tile, me_ref, gain_ref, gate_ref, lin_ref, *refs):
    halves, sums, out_ref = refs[:2], refs[2:5], refs[5]
    owner = owner_of(me_ref, count // 2, count)
    for start in range(0, out_ref.shape[0], tile):
        here = pl.ds(start, tile)
        terms = expand_terms(whole_rows(halves, here), owner, gain_ref, gate_ref, lin_ref)
        gate, lin, squares = added(tuple(ref[here, :] for ref in sums), terms)
        mean = jnp.sum(squares, axis=1, keepdims=True) / (count * out_ref.shape[1])
        factor = lax.rsqrt(mean + EPSILON)
        out_ref[here, :] = clamped_unit(gate * factor, lin * factor).astype(jnp.bfloat16)


def down_term(values, owner, down_ref):
    width = values.shape[1]
    piece = pl.ds(pl.multiple_of(owner * width, width), width)
    return jnp.dot(values, down_ref[piece, :], preferred_element_type=jnp.float32)


def down_kernel(count, offsets, tile, me_ref, down_ref, *refs):
    blocks, out_ref = refs[:-1], refs[-1]
    owners = [owner_of(me_ref, offset, count) for offset in offsets]
    for start in range(0, out_ref.shape[0], tile):
        here, total = pl.ds(start, tile), None
        for block, owner in zip(blocks, owners):
            term = down_term(block[here, :], owner, down_ref)
            total = term if total is None else total + term
        out_ref[here, :] = total


def result_kernel(count, tile, me_ref, down_ref, top_ref, low_ref, sum_ref, out_ref):
    owner = owner_of(me_ref, count // 2, count)
    for start in range(0, out_ref.shape[0], tile):
        here = pl.ds(start, tile)
        term = down_term(whole_rows((top_ref, low_ref), here), owner, down_ref)
        out_ref[here, :] = (sum_ref[here, :] + term).astype(jnp.bfloat16)


def local_call(kernel, out_shape, operands, flops):
    smem, vmem = pl.BlockSpec(memory_space=pltpu.SMEM), pl.BlockSpec(memory_space=pltpu.VMEM)
    return pl.pallas_call(
        kernel,
        out_shape=out_shape,
        in_specs=[smem] + [vmem] * (len(operands) - 1),
        out_specs=[vmem] * len(out_shape) if isinstance(out_shape, list) else vmem,
        compiler_params=pltpu.CompilerParams(vmem_limit_bytes=24 * 2**20),
        cost_estimate=pl.CostEstimate(flops=flops, bytes_accessed=2**22, transcendentals=0),
    )(*operands)


def shards(
    glu_value,
    glu_gate,
    segments,
    conv_kernel,
    norm_gain,
    norm_bias,
    residual,
    out_weight,
    rms_gain,
    experts,
    route_weights,
    glu_weight,
    lin_weight,
    down_weight,
):
    bf16, f32 = jnp.bfloat16, jnp.float32
    tok_count, local_width = glu_value.shape
    model_width = out_weight.shape[1]
    reach = conv_kernel.shape[0] - 1
    top_count = experts.shape[1]
    sp_count, tp_count = lax.axis_size("sp"), lax.axis_size("tp")
    expert_total = glu_weight.shape[0] * sp_count
    capacity = min(tok_count, 2 * tok_count * top_count // expert_total)
    way = 1 - 2 * (lax.axis_index("sp") % 2)
    me = jnp.stack([lax.axis_index("tp"), way]).astype(jnp.int32)
    me, glu_value = lax.optimization_barrier((me, glu_value))

    glu_out = (glu_value.astype(f32) * jax.nn.sigmoid(glu_gate.astype(f32))).astype(bf16)
    last_docs = jnp.pad(segments[tok_count - reach :].astype(bf16), (0, local_width - reach))
    tail = jnp.concatenate([glu_out[tok_count - reach :], last_docs[None, :]], axis=0)
    before = lax.ppermute(tail, "sp", [(i, i + 1) for i in range(sp_count - 1)])
    prev_rows, prev_segments = before[:reach], before[reach, :reach].astype(jnp.int32)

    each = jnp.arange(expert_total, dtype=jnp.int32)
    named = experts[:, :, None] == each
    one_hot = jnp.any(named, axis=1)
    weight_of = jnp.sum(jnp.where(named, route_weights[:, :, None], 0.0), axis=1)
    position = jnp.arange(tok_count, dtype=jnp.int32)
    earlier = (position[:, None] > position[None, :]).astype(bf16)
    rank = jnp.dot(earlier, one_hot.astype(bf16), preferred_element_type=f32)
    rank = jnp.where(one_hot, rank, -1.0).astype(bf16)
    column = jnp.arange(expert_total * capacity, dtype=jnp.int32)
    spread = (each[:, None] == column[None, :] // capacity).astype(bf16)
    rank_of = jnp.dot(rank, spread, preferred_element_type=f32)
    weight_at = jnp.dot(weight_of, spread.astype(f32), precision=lax.Precision.HIGHEST)
    pick = rank_of == (column % capacity).astype(f32)
    weight = jnp.where(pick, weight_at, 0.0)
    upper = lax.reduce_precision(weight, 8, 7)
    weights = (upper.astype(bf16), (weight - upper).astype(bf16))

    padded = jnp.concatenate([prev_rows, glu_out], axis=0).astype(f32)
    padded_segments = jnp.concatenate([prev_segments, segments], axis=0)
    conv_sum = jnp.zeros((tok_count, local_width), f32)
    for offset in range(reach + 1):
        lower = reach - offset
        window_rows = padded[lower : lower + tok_count]
        same_document = (padded_segments[lower : lower + tok_count] == segments).astype(f32)
        conv_sum = conv_sum + conv_kernel[offset][None, :] * window_rows * same_document[:, None]
    sums = jnp.concatenate([jnp.sum(conv_sum, axis=1), jnp.sum(conv_sum * conv_sum, axis=1)])
    totals = everyones_sum(sums, "tp")
    row_mean = totals[:tok_count] / model_width
    row_var = totals[tok_count:] / model_width - row_mean * row_mean
    normed_conv = (conv_sum - row_mean[:, None]) * lax.rsqrt(row_var + EPSILON)[
        :, None
    ] * norm_gain + norm_bias
    swished = jax.nn.silu(normed_conv).astype(bf16)
    projected = jnp.dot(swished, out_weight, preferred_element_type=f32).astype(bf16)
    pieces = lax.all_to_all(in_blocks(projected, 1, tp_count), "tp", 0, 0, tiled=True)
    conv_out = jnp.sum(pieces.astype(f32), axis=0)
    updated = (residual.astype(f32) + conv_out).astype(bf16)

    gain = rms_gain.reshape(tp_count, 1, local_width)
    rows = sp_count * capacity
    packed = lax.dot_general(
        pick.astype(bf16), updated, (((0,), (0,)), ((), ())), preferred_element_type=f32
    ).astype(bf16)
    packed = packed.reshape(sp_count, capacity, local_width)
    arrived = lax.all_to_all(packed, "sp", 0, 0, tiled=True).reshape(rows, local_width)
    tile = min(rows // 2, 256)
    flops = 2 * rows * model_width * local_width
    sums = jax.ShapeDtypeStruct((rows, local_width), f32)
    squares = jax.ShapeDtypeStruct((rows, local_width // 2), f32)
    out = jax.ShapeDtypeStruct((rows, local_width), bf16)
    weights_in = (me, gain, glu_weight[0], lin_weight[0])
    blocks, offsets, last = ring_gather(arrived, ("sp", "tp"))
    expand = functools.partial(expand_kernel, tp_count, offsets, tile)
    partial = local_call(expand, [sums, sums, squares], (*weights_in, *blocks), 2 * flops)
    finish = functools.partial(hidden_kernel, tp_count, tile)
    hidden = local_call(finish, out, (*weights_in, *last, *partial), flops // tp_count)
    blocks, offsets, last = ring_gather(hidden, ("sp", "tp"))
    down = functools.partial(down_kernel, tp_count, offsets, tile)
    partial = local_call(down, sums, (me, down_weight[0], *blocks), flops)
    finish = functools.partial(result_kernel, tp_count, tile)
    result = local_call(finish, out, (me, down_weight[0], *last, partial), flops // tp_count)
    result = result.reshape(sp_count, capacity, local_width)
    returned = lax.all_to_all(result, "sp", 0, 0, tiled=True).reshape(rows, local_width)
    routed = updated.astype(f32)
    for weight in weights:
        routed = routed + jnp.dot(weight, returned, preferred_element_type=f32)
    return routed.astype(bf16)


def solution(mesh):
    in_specs = (
        P(("grp", "sp"), "tp"),
        P(("grp", "sp"), "tp"),
        P(("grp", "sp")),
        P(None, "tp"),
        P("tp"),
        P("tp"),
        P(("grp", "sp"), "tp"),
        P("tp", None),
        P(),
        P(("grp", "sp"), None),
        P(("grp", "sp"), None),
        P("sp", None, "tp"),
        P("sp", None, "tp"),
        P("sp", None, "tp"),
    )
    out_specs = P(("grp", "sp"), "tp")
    return jax.shard_map(shards, mesh=mesh, in_specs=in_specs, out_specs=out_specs, check_vma=False)
```

```python
import functools

import jax
import jax.numpy as jnp
from jax import lax
from jax.experimental import pallas as pl
from jax.experimental.pallas import tpu as pltpu
from jax.sharding import PartitionSpec as P

EPSILON = 1e-05
CLAMP_LIMIT = 7.0
SIGMOID_SCALE = 1.702
PARTS = 2


def shifted(array, axis, by):
    length = lax.axis_size(axis)
    return lax.ppermute(array, axis, [(i, (i + by) % length) for i in range(length)])


def ring_gather(own, axis, flip):
    length = lax.axis_size(axis)
    step = -1 if flip else 1
    blocks, offsets = [own], [0]
    ahead = back = own
    for hop in range(1, length // 2 + 1):
        ahead = shifted(ahead, axis, step)
        blocks.append(ahead)
        offsets.append(-step * hop)
        if hop < length - length // 2:
            back = shifted(back, axis, -step)
            blocks.append(back)
            offsets.append(step * hop)
    return blocks, tuple(offsets)


def in_blocks(array, dim, length):
    lengths = array.shape
    blocks = array.reshape(*lengths[:dim], length, lengths[dim] // length, *lengths[dim + 1 :])
    return jnp.moveaxis(blocks, dim, 0)


def everyones_sum(array, axis):
    copies = jnp.broadcast_to(array, (lax.axis_size(axis), *array.shape))
    return lax.all_to_all(copies, axis, split_axis=0, concat_axis=0, tiled=True).sum(axis=0)


def clamped_unit(gate_pre, lin_pre):
    gate_clip = jnp.minimum(gate_pre, CLAMP_LIMIT)
    linear = jnp.clip(lin_pre, -CLAMP_LIMIT, CLAMP_LIMIT)
    return gate_clip * jax.nn.sigmoid(SIGMOID_SCALE * gate_clip) * (linear + 1.0)


def owners_of(me_ref, offsets):
    count = len(offsets)
    return [lax.rem(me_ref[0] + offset + count, count) for offset in offsets]


def piece_of(owner, width):
    return pl.ds(pl.multiple_of(owner * width, width), width)


def hidden_kernel(offsets, tile, me_ref, gain_ref, gate_ref, lin_ref, *refs):
    blocks, out_ref = refs[:-1], refs[-1]
    rows, width = blocks[0].shape
    owners = owners_of(me_ref, offsets)
    for start in range(0, rows, tile):
        here, totals = pl.ds(start, tile), None
        for block, owner in zip(blocks, owners):
            piece = piece_of(owner, width)
            values = block[here, :].astype(jnp.float32)
            scaled = (values * gain_ref[owner]).astype(jnp.bfloat16)
            gate = jnp.dot(scaled, gate_ref[piece, :], preferred_element_type=jnp.float32)
            lin = jnp.dot(scaled, lin_ref[piece, :], preferred_element_type=jnp.float32)
            square = values * values
            terms = gate, lin, square[:, : width // 2] + square[:, width // 2 :]
            totals = terms if totals is None else tuple(a + b for a, b in zip(totals, terms))
        gate, lin, squares = totals
        mean = jnp.sum(squares, axis=1, keepdims=True) / (len(offsets) * width)
        factor = lax.rsqrt(mean + EPSILON)
        out_ref[here, :] = clamped_unit(gate * factor, lin * factor).astype(jnp.bfloat16)


def down_kernel(offsets, tile, me_ref, down_ref, *refs):
    blocks, results, out_ref = refs[: len(offsets)], refs[len(offsets) : -1], refs[-1]
    rows, width = blocks[0].shape
    owners = owners_of(me_ref, offsets)
    ahead = 0
    for result in results:
        out_ref[pl.ds(ahead, result.shape[0]), :] = result[...]
        ahead += result.shape[0]
    for start in range(0, rows, tile):
        total = None
        for block, owner in zip(blocks, owners):
            weight = down_ref[piece_of(owner, width), :]
            values = block[pl.ds(start, tile), :]
            term = jnp.dot(values, weight, preferred_element_type=jnp.float32)
            total = term if total is None else total + term
        out_ref[pl.ds(ahead + start, tile), :] = total.astype(jnp.bfloat16)


def local_call(kernel, out_shape, operands, flops):
    smem, vmem = pl.BlockSpec(memory_space=pltpu.SMEM), pl.BlockSpec(memory_space=pltpu.VMEM)
    return pl.pallas_call(
        kernel,
        out_shape=out_shape,
        in_specs=[smem] + [vmem] * (len(operands) - 1),
        out_specs=vmem,
        compiler_params=pltpu.CompilerParams(vmem_limit_bytes=24 * 2**20),
        cost_estimate=pl.CostEstimate(flops=flops, bytes_accessed=2**22, transcendentals=0),
    )(*operands)


def shards(
    glu_value,
    glu_gate,
    segments,
    conv_kernel,
    norm_gain,
    norm_bias,
    residual,
    out_weight,
    rms_gain,
    experts,
    route_weights,
    glu_weight,
    lin_weight,
    down_weight,
):
    bf16, f32 = jnp.bfloat16, jnp.float32
    tok_count, local_width = glu_value.shape
    model_width = out_weight.shape[1]
    reach = conv_kernel.shape[0] - 1
    top_count = experts.shape[1]
    sp_count, tp_count = lax.axis_size("sp"), lax.axis_size("tp")
    expert_total = glu_weight.shape[0] * sp_count
    capacity = min(tok_count, 2 * tok_count * top_count // expert_total)
    me = lax.axis_index("tp").astype(jnp.int32).reshape(1)
    me, glu_value = lax.optimization_barrier((me, glu_value))

    glu_out = (glu_value.astype(f32) * jax.nn.sigmoid(glu_gate.astype(f32))).astype(bf16)
    last_docs = jnp.pad(segments[tok_count - reach :].astype(bf16), (0, local_width - reach))
    tail = jnp.concatenate([glu_out[tok_count - reach :], last_docs[None, :]], axis=0)
    before = lax.ppermute(tail, "sp", [(i, i + 1) for i in range(sp_count - 1)])
    prev_rows, prev_segments = before[:reach], before[reach, :reach].astype(jnp.int32)

    each = jnp.arange(expert_total, dtype=jnp.int32)
    named = experts[:, :, None] == each
    one_hot = jnp.any(named, axis=1)
    weight_of = jnp.sum(jnp.where(named, route_weights[:, :, None], 0.0), axis=1)
    position = jnp.arange(tok_count, dtype=jnp.int32)
    earlier = (position[:, None] > position[None, :]).astype(bf16)
    rank = jnp.dot(earlier, one_hot.astype(bf16), preferred_element_type=f32)
    rank = jnp.where(one_hot, rank, -1.0).astype(bf16)
    column = jnp.arange(expert_total * capacity, dtype=jnp.int32)
    spread = (each[:, None] == column[None, :] // capacity).astype(bf16)
    rank_of = jnp.dot(rank, spread, preferred_element_type=f32)
    weight_at = jnp.dot(weight_of, spread.astype(f32), precision=lax.Precision.HIGHEST)
    pick = rank_of == (column % capacity).astype(f32)
    weight = jnp.where(pick, weight_at, 0.0)
    upper = lax.reduce_precision(weight, 8, 7)
    weights = (upper.astype(bf16), (weight - upper).astype(bf16))

    padded = jnp.concatenate([prev_rows, glu_out], axis=0).astype(f32)
    padded_segments = jnp.concatenate([prev_segments, segments], axis=0)
    conv_sum = jnp.zeros((tok_count, local_width), f32)
    for offset in range(reach + 1):
        lower = reach - offset
        window_rows = padded[lower : lower + tok_count]
        same_document = (padded_segments[lower : lower + tok_count] == segments).astype(f32)
        conv_sum = conv_sum + conv_kernel[offset][None, :] * window_rows * same_document[:, None]
    sums = jnp.concatenate([jnp.sum(conv_sum, axis=1), jnp.sum(conv_sum * conv_sum, axis=1)])
    totals = everyones_sum(sums, "tp")
    row_mean = totals[:tok_count] / model_width
    row_var = totals[tok_count:] / model_width - row_mean * row_mean
    normed_conv = (conv_sum - row_mean[:, None]) * lax.rsqrt(row_var + EPSILON)[
        :, None
    ] * norm_gain + norm_bias
    swished = jax.nn.silu(normed_conv).astype(bf16)
    projected = jnp.dot(swished, out_weight, preferred_element_type=f32).astype(bf16)
    pieces = lax.all_to_all(in_blocks(projected, 1, tp_count), "tp", 0, 0, tiled=True)
    conv_out = jnp.sum(pieces.astype(f32), axis=0)
    updated = (residual.astype(f32) + conv_out).astype(bf16)

    gain = rms_gain.reshape(tp_count, 1, local_width)
    rows = sp_count * capacity
    packed = lax.dot_general(
        pick.astype(bf16), updated, (((0,), (0,)), ((), ())), preferred_element_type=f32
    ).astype(bf16)
    packed = packed.reshape(sp_count, capacity, local_width)
    arrived = lax.all_to_all(packed, "sp", 0, 0, tiled=True).reshape(rows, local_width)
    part_rows = rows // PARTS
    out_block = jax.ShapeDtypeStruct((part_rows, local_width), bf16)
    flops = 2 * part_rows * model_width * local_width
    tile = min(part_rows, 256)
    hidden, results = [], []
    for part in range(PARTS):
        own = arrived[part * part_rows : (part + 1) * part_rows]
        blocks, offsets = ring_gather(own, "tp", part % 2)
        hidden.append(
            local_call(
                functools.partial(hidden_kernel, offsets, tile),
                out_block,
                (me, gain, glu_weight[0], lin_weight[0], *blocks),
                2 * flops,
            )
        )
    for part in range(PARTS):
        blocks, offsets = ring_gather(hidden[part], "tp", part % 2)
        results = [
            local_call(
                functools.partial(down_kernel, offsets, tile),
                jax.ShapeDtypeStruct(((part + 1) * part_rows, local_width), bf16),
                (me, down_weight[0], *blocks, *results),
                flops,
            )
        ]
    result = results[0].reshape(sp_count, capacity, local_width)
    returned = lax.all_to_all(result, "sp", 0, 0, tiled=True).reshape(rows, local_width)
    routed = updated.astype(f32)
    for weight in weights:
        routed = routed + jnp.dot(weight, returned, preferred_element_type=f32)
    return routed.astype(bf16)


def solution(mesh):
    in_specs = (
        P(("grp", "sp"), "tp"),
        P(("grp", "sp"), "tp"),
        P(("grp", "sp")),
        P(None, "tp"),
        P("tp"),
        P("tp"),
        P(("grp", "sp"), "tp"),
        P("tp", None),
        P(),
        P(("grp", "sp"), None),
        P(("grp", "sp"), None),
        P("sp", None, "tp"),
        P("sp", None, "tp"),
        P("sp", None, "tp"),
    )
    out_specs = P(("grp", "sp"), "tp")
    return jax.shard_map(shards, mesh=mesh, in_specs=in_specs, out_specs=out_specs, check_vma=False)
```

```python
import functools

import jax
import jax.numpy as jnp
from jax import lax
from jax.experimental import pallas as pl
from jax.experimental.pallas import tpu as pltpu
from jax.sharding import PartitionSpec as P

EPSILON = 1e-05
CLAMP_LIMIT = 7.0
SIGMOID_SCALE = 1.702
PARTS = 2


def shifted(array, axis, by):
    length = lax.axis_size(axis)
    return lax.ppermute(array, axis, [(i, (i + by) % length) for i in range(length)])


def ring_gather(own, axis, flip):
    length = lax.axis_size(axis)
    step = -1 if flip else 1
    blocks, offsets = [own], [0]
    ahead = back = own
    for hop in range(1, length // 2 + 1):
        ahead = shifted(ahead, axis, step)
        blocks.append(ahead)
        offsets.append(-step * hop)
        if hop < length - length // 2:
            back = shifted(back, axis, -step)
            blocks.append(back)
            offsets.append(step * hop)
    return blocks, tuple(offsets)


def project_kernel(model_width, totals_ref, scale_ref, sums_ref, weight_ref, out_ref):
    rows, width = sums_ref.shape
    totals = jnp.sum(totals_ref[...], axis=0) / model_width
    here = lax.broadcasted_iota(jnp.int32, (rows, rows), 0)
    same = here == lax.broadcasted_iota(jnp.int32, (rows, rows), 1)
    mean = jnp.sum(jnp.where(same, totals[:, :rows], 0.0), axis=1, keepdims=True)
    square = jnp.sum(jnp.where(same, totals[:, rows:], 0.0), axis=1, keepdims=True)
    factor = lax.rsqrt(square - mean * mean + EPSILON)
    value = (sums_ref[...] - mean) * factor * scale_ref[0:1, :] + scale_ref[1:2, :]
    swished = (value * jax.nn.sigmoid(value)).astype(jnp.bfloat16)
    for block in range(out_ref.shape[0]):
        piece = weight_ref[:, pl.ds(block * width, width)]
        product = jnp.dot(swished, piece, preferred_element_type=jnp.float32)
        out_ref[block] = product.astype(jnp.bfloat16)


def clamped_unit(gate_pre, lin_pre):
    gate_clip = jnp.minimum(gate_pre, CLAMP_LIMIT)
    linear = jnp.clip(lin_pre, -CLAMP_LIMIT, CLAMP_LIMIT)
    return gate_clip * jax.nn.sigmoid(SIGMOID_SCALE * gate_clip) * (linear + 1.0)


def owners_of(me_ref, offsets):
    count = len(offsets)
    return [lax.rem(me_ref[0] + offset + count, count) for offset in offsets]


def piece_of(owner, width):
    return pl.ds(pl.multiple_of(owner * width, width), width)


def hidden_kernel(offsets, tile, me_ref, gain_ref, gate_ref, lin_ref, *refs):
    blocks, out_ref = refs[:-1], refs[-1]
    rows, width = blocks[0].shape
    owners = owners_of(me_ref, offsets)
    for start in range(0, rows, tile):
        here, totals = pl.ds(start, tile), None
        for block, owner in zip(blocks, owners):
            piece = piece_of(owner, width)
            values = block[here, :].astype(jnp.float32)
            scaled = (values * gain_ref[owner]).astype(jnp.bfloat16)
            gate = jnp.dot(scaled, gate_ref[piece, :], preferred_element_type=jnp.float32)
            lin = jnp.dot(scaled, lin_ref[piece, :], preferred_element_type=jnp.float32)
            square = values * values
            terms = gate, lin, square[:, : width // 2] + square[:, width // 2 :]
            totals = terms if totals is None else tuple(a + b for a, b in zip(totals, terms))
        gate, lin, squares = totals
        mean = jnp.sum(squares, axis=1, keepdims=True) / (len(offsets) * width)
        factor = lax.rsqrt(mean + EPSILON)
        out_ref[here, :] = clamped_unit(gate * factor, lin * factor).astype(jnp.bfloat16)


def down_kernel(offsets, tile, me_ref, down_ref, *refs):
    blocks, results, out_ref = refs[: len(offsets)], refs[len(offsets) : -1], refs[-1]
    rows, width = blocks[0].shape
    owners = owners_of(me_ref, offsets)
    for part, result in enumerate(results):
        out_ref[:, part] = result[...].reshape(-1, *out_ref.shape[2:])
    for start in range(0, rows, tile):
        total = None
        for block, owner in zip(blocks, owners):
            weight = down_ref[piece_of(owner, width), :]
            values = block[pl.ds(start, tile), :]
            term = jnp.dot(values, weight, preferred_element_type=jnp.float32)
            total = term if total is None else total + term
        total = total.astype(jnp.bfloat16)
        if results:
            slots = out_ref.shape[2]
            chips = pl.ds(start // slots, tile // slots)
            out_ref[chips, len(results)] = total.reshape(-1, *out_ref.shape[2:])
        else:
            out_ref[pl.ds(start, tile), :] = total


def local_call(kernel, out_shape, operands, flops):
    smem, vmem = pl.BlockSpec(memory_space=pltpu.SMEM), pl.BlockSpec(memory_space=pltpu.VMEM)
    return pl.pallas_call(
        kernel,
        out_shape=out_shape,
        in_specs=[smem] + [vmem] * (len(operands) - 1),
        out_specs=vmem,
        compiler_params=pltpu.CompilerParams(vmem_limit_bytes=24 * 2**20),
        cost_estimate=pl.CostEstimate(flops=flops, bytes_accessed=2**22, transcendentals=0),
    )(*operands)


def shards(
    glu_value,
    glu_gate,
    segments,
    conv_kernel,
    norm_gain,
    norm_bias,
    residual,
    out_weight,
    rms_gain,
    experts,
    route_weights,
    glu_weight,
    lin_weight,
    down_weight,
):
    bf16, f32 = jnp.bfloat16, jnp.float32
    tok_count, local_width = glu_value.shape
    model_width = out_weight.shape[1]
    reach = conv_kernel.shape[0] - 1
    top_count = experts.shape[1]
    sp_count, tp_count = lax.axis_size("sp"), lax.axis_size("tp")
    expert_total = glu_weight.shape[0] * sp_count
    capacity = min(tok_count, 2 * tok_count * top_count // expert_total)
    core = (lax.axis_index("sp") % PARTS).astype(jnp.int32)
    me = lax.axis_index("tp").astype(jnp.int32).reshape(1)
    scale = jnp.stack([norm_gain, norm_bias])
    me, core, scale, glu_value = lax.optimization_barrier((me, core, scale, glu_value))
    sides = [[i for i in range(sp_count) if i % PARTS == c] for c in range(PARTS)]

    glu_out = (glu_value.astype(f32) * jax.nn.sigmoid(glu_gate.astype(f32))).astype(bf16)
    last_docs = jnp.pad(segments[tok_count - reach :].astype(bf16), (0, local_width - reach))
    tail = jnp.concatenate([glu_out[tok_count - reach :], last_docs[None, :]], axis=0)
    before = lax.ppermute(tail, "sp", [(i, i + 1) for i in range(sp_count - 1)])
    prev_rows, prev_segments = before[:reach], before[reach, :reach].astype(jnp.int32)

    each = jnp.arange(expert_total, dtype=jnp.int32)
    named = experts[:, :, None] == each
    one_hot = jnp.any(named, axis=1)
    weight_of = jnp.sum(jnp.where(named, route_weights[:, :, None], 0.0), axis=1)
    position = jnp.arange(tok_count, dtype=jnp.int32)
    earlier = (position[:, None] > position[None, :]).astype(bf16)
    rank = jnp.dot(earlier, one_hot.astype(bf16), preferred_element_type=f32)
    rank = jnp.where(one_hot, rank, -1.0).astype(bf16)
    column = jnp.arange(expert_total * capacity, dtype=jnp.int32)
    at_slot = (column // capacity + core * (1 - 2 * (column // capacity % PARTS))).astype(jnp.int32)
    spread = (each[:, None] == at_slot[None, :]).astype(bf16)
    rank_of = jnp.dot(rank, spread, preferred_element_type=f32)
    weight_at = jnp.dot(weight_of, spread.astype(f32), precision=lax.Precision.HIGHEST)
    pick = rank_of == (column % capacity).astype(f32)
    weight = jnp.where(pick, weight_at, 0.0)
    upper = lax.reduce_precision(weight, 8, 7)
    weights = (upper.astype(bf16), (weight - upper).astype(bf16))

    padded = jnp.concatenate([prev_rows, glu_out], axis=0).astype(f32)
    padded_segments = jnp.concatenate([prev_segments, segments], axis=0)
    conv_sum = jnp.zeros((tok_count, local_width), f32)
    for offset in range(reach + 1):
        lower = reach - offset
        window_rows = padded[lower : lower + tok_count]
        same_document = (padded_segments[lower : lower + tok_count] == segments).astype(f32)
        conv_sum = conv_sum + conv_kernel[offset][None, :] * window_rows * same_document[:, None]
    sums = jnp.concatenate([jnp.sum(conv_sum, axis=1), jnp.sum(conv_sum * conv_sum, axis=1)])
    copies = jnp.broadcast_to(sums, (tp_count, 1, sums.size))
    totals = lax.all_to_all(copies, "tp", 0, 0, tiled=True)
    projected = pl.pallas_call(
        functools.partial(project_kernel, model_width),
        out_shape=jax.ShapeDtypeStruct((tp_count, tok_count, local_width), bf16),
        compiler_params=pltpu.CompilerParams(vmem_limit_bytes=24 * 2**20),
        cost_estimate=pl.CostEstimate(
            flops=2 * tok_count * local_width * model_width,
            bytes_accessed=2**21,
            transcendentals=0,
        ),
    )(totals, scale, conv_sum, out_weight)
    swap = [(i, i + 1 - 2 * (i % PARTS)) for i in range(sp_count)]
    ours = (glu_weight[0], lin_weight[0], down_weight[0])
    projected, *tied = lax.optimization_barrier((projected, *ours))
    pieces = lax.all_to_all(projected, "tp", 0, 0, tiled=True)
    others = [lax.ppermute(weight, "sp", swap) for weight in tied]
    pieces, *others = lax.optimization_barrier((pieces, *others))
    glu_parts, lin_parts, down_parts = zip(ours, others)
    conv_out = jnp.sum(pieces.astype(f32), axis=0)
    updated = (residual.astype(f32) + conv_out).astype(bf16)

    gain = rms_gain.reshape(tp_count, 1, local_width)
    rows = sp_count * capacity
    packed = lax.dot_general(
        pick.astype(bf16), updated, (((0,), (0,)), ((), ())), preferred_element_type=f32
    ).astype(bf16)
    chips = sp_count // PARTS
    packed = packed.reshape(chips, PARTS, capacity, local_width)
    arrived = lax.all_to_all(packed, "sp", 0, 0, tiled=True, axis_index_groups=sides)
    part_rows = chips * capacity
    out_block = jax.ShapeDtypeStruct((part_rows, local_width), bf16)
    out = jax.ShapeDtypeStruct((chips, PARTS, capacity, local_width), bf16)
    flops = 2 * part_rows * model_width * local_width
    tile = min(part_rows, 256)
    hidden, results = [], []
    for part in range(PARTS):
        own = arrived[:, part].reshape(part_rows, local_width)
        blocks, offsets = ring_gather(own, "tp", part % 2)
        hidden.append(
            local_call(
                functools.partial(hidden_kernel, offsets, tile),
                out_block,
                (me, gain, glu_parts[part], lin_parts[part], *blocks),
                2 * flops,
            )
        )
    for part in range(PARTS):
        blocks, offsets = ring_gather(hidden[part], "tp", part % 2)
        results = [
            local_call(
                functools.partial(down_kernel, offsets, tile),
                out if part else out_block,
                (me, down_parts[part], *blocks, *results),
                flops,
            )
        ]
    returned = lax.all_to_all(results[0], "sp", 0, 0, tiled=True, axis_index_groups=sides)
    returned = returned.reshape(rows, local_width)
    routed = updated.astype(f32)
    for weight in weights:
        routed = routed + jnp.dot(weight, returned, preferred_element_type=f32)
    return routed.astype(bf16)


def solution(mesh):
    in_specs = (
        P(("grp", "sp"), "tp"),
        P(("grp", "sp"), "tp"),
        P(("grp", "sp")),
        P(None, "tp"),
        P("tp"),
        P("tp"),
        P(("grp", "sp"), "tp"),
        P("tp", None),
        P(),
        P(("grp", "sp"), None),
        P(("grp", "sp"), None),
        P("sp", None, "tp"),
        P("sp", None, "tp"),
        P("sp", None, "tp"),
    )
    out_specs = P(("grp", "sp"), "tp")
    return jax.shard_map(shards, mesh=mesh, in_specs=in_specs, out_specs=out_specs, check_vma=False)
```
